32 devices in a mesh: ep: 8 (over z, y), tp: 4 (over x, core).
Axes of the slice: x: 2, y: 2, z: 4, core: 2. Of those that a mesh axis runs over, the one named last changes fastest.
Arguments:
- tokens: bfloat16 [1792, 2048], P('ep'), may hold values from -6 to 6
- cotangent: bfloat16 [1792, 2048], P('ep'), may hold values from -6 to 6
- routes: int32 [1792, 2], P('ep'), may hold values from 0 to 7, all different within a row; in each aligned block of 224 rows (0 to 223, 224 to 447, ...) at most 112 rows name the same one
- gate_weights: float32 [1792, 2], P('ep'), may hold values from 0.2 to 1
- w_gate: bfloat16 [8, 2048, 1792], P('ep', None, 'tp'), may hold values from -0.125 to 0.125
- w_up: bfloat16 [8, 2048, 1792], P('ep', None, 'tp'), may hold values from -0.125 to 0.125
- w_down: bfloat16 [8, 1792, 2048], P('ep', 'tp'), may hold values from -0.125 to 0.125
Outputs:
- token_grad: bfloat16 [1792, 2048], P('ep', 'tp')
- score_grad: float32 [1792, 2], P('ep')
- gate_grad: bfloat16 [8, 2048, 1792], P('ep', None, 'tp')
- up_grad: bfloat16 [8, 2048, 1792], P('ep', None, 'tp')
- down_grad: bfloat16 [8, 1792, 2048], P('ep', 'tp')
- row_norms: float32 [2048], replicated
The draws below stay inside these ranges and needn't reach their ends.
Inputs may be any that keep to these rules, and one draw needn't show every extreme that they name: `routes`: within the rows of one device, no expert is named by more than 112 of the pairs; some expert is named by exactly 112 of them in some blocks. The 2 experts of a token differ.
All inputs are finite; a program needn't handle non-finite values.
Results may differ from the reference program's by a relative error of at most 0.014.
Values may be sent and summed in bfloat16 or wider, within the bound.
A program may use at most 128 MiB of HBM per device.

```python
import math
import jax
import jax.numpy as jnp
import numpy as np
from jax import lax

D = 2048
FF = 1792
TOP = 2
TOK_DEV = 224
EXPERTS = 8
CAP = 112
TOKENS = 1792
N_EP = 8
N_TP = 4


def steps_of(own_key, extent, cuts, low, high):
    level, own = 1.0, jax.random.fold_in(own_key, 6)
    for dim, shards_of in cuts:
        heights = jnp.exp(jax.random.uniform(jax.random.fold_in(own, dim), (shards_of,), jnp.float32, low / len(cuts), high / len(cuts)))
        level = level * jnp.repeat(heights, extent[dim] // shards_of).reshape([-1 if axis == dim else 1 for axis in range(len(extent))])
    return level


def routed_block(rng, own, number, rows, number_of, top, bound, slope):
    order = jax.random.permutation(rng, number_of)
    packed, usual = load_shares(number_of, rows * top, bound, slope, True), load_shares(number_of, rows * top, bound, slope, False)
    places = jnp.arange(number_of)

    def named(tallies, turn):
        used = int((tallies > 0).sum())
        fixed = max(1, used // 4)
        moved = fixed + (places - fixed + turn * (used - fixed)) % max(1, number_of - fixed)
        return jnp.zeros((number_of,), jnp.int32).at[order[jnp.where(places < fixed, places, moved)]].set(jnp.asarray(tallies, jnp.int32))

    tallies = jnp.where(number % 4 == 0, named(packed, number // 4), named(usual, number - number // 4 - 1))
    mixed = jax.random.permutation(jax.random.fold_in(own, 3), number_of)
    donor, sink = mixed[0:number_of // 2 * 2:2], mixed[1:number_of // 2 * 2:2]
    slack = jnp.minimum(tallies[donor] - 1, bound - tallies[sink]) // 2
    slack = jnp.where((donor == order[0]) | (sink == order[0]) | (tallies[sink] == 0), 0, jnp.maximum(slack, 0))
    moved = jax.random.randint(jax.random.fold_in(own, 4), (number_of // 2,), 0, 1 << 20) % (slack + 1)
    tallies = tallies.at[donor].add(-moved).at[sink].add(moved)
    items = jnp.searchsorted(jnp.cumsum(tallies), jnp.arange(rows * top), side="right").astype(jnp.int32)
    table = items.reshape(top, rows).T
    table = table[jax.random.permutation(jax.random.fold_in(own, 1), rows)]
    turn = jax.random.randint(jax.random.fold_in(own, 2), (rows, 1), 0, top)
    return jnp.take_along_axis(table, (jnp.arange(top)[None, :] + turn) % top, axis=1)


def load_shares(amount, total, reach, slope, full):
    loads = [(1 << 20) // math.isqrt(grade ** slope) + 1 for grade in range(1, amount + 1)]
    largest = reach if full else min(reach, max(-(-total // amount), total * loads[0] // sum(loads)))
    least = 1 if total - largest >= amount - 1 else 0
    given, rest = [largest] + [least] * (amount - 1), total - largest - least * (amount - 1)
    while rest > 0:
        free = [i for i in range(1, amount) if given[i] < largest] or [i for i in range(1, amount) if given[i] < reach]
        pool, left = sum([loads[i] for i in free]), rest
        for i in free:
            addition = min(reach - given[i], max(1, left * loads[i] // pool), rest)
            given[i] = given[i] + addition
            rest = rest - addition
    return np.array(given)


def scatter_about(own_key, extent, scale, limit, shards=(), held_as=jnp.bfloat16):
    entries = scale * jax.random.normal(own_key, extent, jnp.float32)
    if shards:
        entries = entries * steps_of(own_key, extent, shards, -0.22, 0.18)
    return jnp.clip(entries, -limit, limit).astype(held_as)


def setup_inputs(seed: int = 0) -> dict:
    key_of = jax.random.split(jax.random.key(seed), 8)
    tokens = scatter_about(key_of[0], (TOKENS, D), 1.0, 6.0, ((0, 8),))
    cotangent = scatter_about(key_of[1], (TOKENS, D), 1.0, 6.0, ((0, 8),))
    routes_keys = jax.random.split(jax.random.fold_in(key_of[2], 1), TOKENS // TOK_DEV)
    routes_turns = jax.random.permutation(jax.random.fold_in(key_of[2], 3), TOKENS // TOK_DEV)
    routes = jax.vmap(lambda own, number: routed_block(jax.random.fold_in(key_of[2], 2), own, number, TOK_DEV, EXPERTS, TOP, CAP, 2))(routes_keys, routes_turns).reshape((TOKENS, TOP))
    gate_weights = jnp.clip(0.2 + 0.8 * jax.random.uniform(key_of[3], (TOKENS, TOP), jnp.float32) ** steps_of(key_of[3], (TOKENS, TOP), ((0, 8),), -0.2, 0.2), 0.2, 1.0)
    w_gate = scatter_about(key_of[4], (EXPERTS, D, FF), D ** -0.5, 0.125, ((0, 8), (2, 4)))
    w_up = scatter_about(key_of[5], (EXPERTS, D, FF), D ** -0.5, 0.125, ((0, 8), (2, 4)))
    w_down = scatter_about(key_of[6], (EXPERTS, FF, D), FF ** -0.5, 0.125, ((0, 8), (1, 4)))
    return dict(tokens=tokens, cotangent=cotangent, routes=routes, gate_weights=gate_weights, w_gate=w_gate, w_up=w_up, w_down=w_down)


def place(block_routes, experts, capacity):
    flat = block_routes.reshape(-1).astype(jnp.int32)
    onehot = (flat[:, None] == jnp.arange(experts, dtype=jnp.int32)[None, :]).astype(jnp.int32)
    before = jnp.cumsum(onehot, axis=0) - onehot
    position = jnp.sum(before * onehot, axis=1).astype(jnp.int32)
    return (flat * capacity + position).astype(jnp.int32)


def reference(tokens, cotangent, routes, gate_weights, w_gate, w_up, w_down):
    items = TOKENS * TOP
    slot_index = jax.vmap(lambda block: place(block, EXPERTS, CAP))(routes.reshape(N_EP, TOK_DEV * TOP))
    item_ids = jnp.arange(items, dtype=jnp.int32).reshape(N_EP, TOK_DEV * TOP)
    empty = jnp.full((N_EP, EXPERTS * CAP), items, jnp.int32)
    table = jax.vmap(lambda base, where, ids: base.at[where].set(ids))(empty, slot_index, item_ids)
    table = table.reshape(N_EP, EXPERTS, CAP).transpose(1, 0, 2).reshape(EXPERTS, N_EP * CAP)
    tokens_pad = jnp.concatenate([tokens, jnp.zeros((1, D), tokens.dtype)], axis=0)
    cot_pad = jnp.concatenate([cotangent, jnp.zeros((1, D), cotangent.dtype)], axis=0)
    gates_pad = jnp.concatenate([gate_weights.reshape(-1), jnp.zeros((1,), jnp.float32)])
    gates_low = lax.optimization_barrier(gates_pad.astype(jnp.bfloat16)).astype(jnp.float32)
    group = FF // N_TP

    def expert_step(carry, inputs):
        grad_acc, score_acc = carry
        item, wg, wu, wd = inputs
        row = (item // TOP).astype(jnp.int32)
        x_rows = tokens_pad[row]
        c_rows = cot_pad[row]
        scale = gates_low[item][:, None]
        pre_gate = jnp.dot(x_rows, wg, preferred_element_type=jnp.float32)
        pre_up = jnp.dot(x_rows, wu, preferred_element_type=jnp.float32)
        sig = jax.nn.sigmoid(pre_gate)
        act = pre_gate * sig
        hidden = (act * pre_up).astype(jnp.bfloat16)
        back = jnp.dot(c_rows, wd.T, preferred_element_type=jnp.float32)
        scaled = scale * back
        d_out = (scale * c_rows.astype(jnp.float32)).astype(jnp.bfloat16)
        d_gate_pre = (scaled * pre_up * sig * (1.0 + pre_gate * (1.0 - sig))).astype(jnp.bfloat16)
        d_up_pre = (scaled * act).astype(jnp.bfloat16)
        grad_down = jnp.dot(hidden.T, d_out, preferred_element_type=jnp.float32).astype(jnp.bfloat16)
        grad_gate = jnp.dot(x_rows.T, d_gate_pre, preferred_element_type=jnp.float32).astype(jnp.bfloat16)
        grad_up = jnp.dot(x_rows.T, d_up_pre, preferred_element_type=jnp.float32).astype(jnp.bfloat16)
        route_grad = jnp.zeros((x_rows.shape[0], D), jnp.float32)
        route_score = jnp.zeros((x_rows.shape[0],), jnp.float32)
        hidden_wide = hidden.astype(jnp.float32)
        for j in range(N_TP):
            lo = j * group
            hi = lo + group
            piece = jnp.dot(d_gate_pre[:, lo:hi], wg[:, lo:hi].T, preferred_element_type=jnp.float32)
            piece = piece + jnp.dot(d_up_pre[:, lo:hi], wu[:, lo:hi].T, preferred_element_type=jnp.float32)
            route_grad = route_grad + piece.astype(jnp.bfloat16).astype(jnp.float32)
            partial_score = jnp.sum(hidden_wide[:, lo:hi] * back[:, lo:hi], axis=1)
            route_score = route_score + partial_score.astype(jnp.bfloat16).astype(jnp.float32)
        route_grad = route_grad.astype(jnp.bfloat16).astype(jnp.float32)
        route_score = route_score.astype(jnp.bfloat16).astype(jnp.float32)
        grad_acc = grad_acc.at[row].add(route_grad)
        score_acc = score_acc.at[item].add(route_score)
        gate_wide = grad_gate.astype(jnp.float32)
        up_wide = grad_up.astype(jnp.float32)
        norms = jnp.sum(gate_wide * gate_wide + up_wide * up_wide, axis=1)
        return (grad_acc, score_acc), (grad_gate, grad_up, grad_down, norms)

    start = (jnp.zeros((TOKENS + 1, D), jnp.float32), jnp.zeros((items + 1,), jnp.float32))
    (grad_acc, score_acc), (gate_grad, up_grad, down_grad, norms) = lax.scan(
        expert_step, start, (table, w_gate, w_up, w_down))
    token_grad = grad_acc[:TOKENS].astype(jnp.bfloat16)
    score_grad = score_acc[:items].reshape(TOKENS, TOP)
    return token_grad, score_grad, gate_grad, up_grad, down_grad, jnp.sum(norms, axis=0)
```

```python
import functools

import jax
import jax.numpy as jnp
from jax import lax
from jax.experimental import pallas as pl
from jax.experimental.pallas import tpu as pltpu
from jax.sharding import PartitionSpec as P

MESH = pl.DeviceIdType.MESH
F32 = jnp.float32
BF = jnp.bfloat16
INNER = (((1,), (1,)), ((), ()))
OUTER = (((0,), (0,)), ((), ()))
PAD = 16
EXTRA = 2


def kernel(n, sel, tok, cot, wg_h, wu_h, wd_h, ret, gg, gu, gd, nout,
           wg, wu, wd, xs, xd, hid, da_s, du_s, part, ra, rb, sb, fb, nrow, ntp, nep,
           wsem, ssem, rsem, ntps, ntpr, neps, nepr):
    me = lax.axis_index("ep")
    j = lax.axis_index("tp")
    sib = j + 1 - 2 * lax.rem(j, 2)
    far = lax.rem(j + 2, 4)
    farsib = lax.rem(sib + 2, 4)
    cap = xd.shape[2]
    width = xd.shape[3]
    quarter = width // 4
    extra = EXTRA * 128
    rest = quarter - extra
    chunk = 256
    chunks = width // chunk

    weights = [pltpu.make_async_copy(src, dst, wsem.at[k])
               for k, (src, dst) in enumerate(((wg_h, wg), (wu_h, wu), (wd_h, wd)))]
    for w in weights:
        w.start()

    barrier = pltpu.get_barrier_semaphore()

    def greet(s, carry):
        pl.semaphore_signal(barrier, inc=1, device_id=(lax.rem(me + s, n), j), device_id_type=MESH)
        return carry

    lax.fori_loop(1, n, greet, 0)
    for k in range(1, 4):
        pl.semaphore_signal(barrier, inc=1, device_id=(me, lax.rem(j + k, 4)), device_id_type=MESH)

    def cols(q, start, size):
        return pl.ds(pl.multiple_of(q * quarter + start, 128), size)

    def copy(src, dst, kind, send_at, recv_at, dev):
        return pltpu.make_async_remote_copy(
            src_ref=src, dst_ref=dst, send_sem=ssem.at[kind, send_at],
            recv_sem=rsem.at[kind, recv_at], device_id=dev, device_id_type=MESH)

    def direct(e, c):
        out = [copy(xs.at[:, e, :, c[0]], xd.at[:, me, :, c[0]], 0, e, me, (e, j))]
        if extra:
            out.append(copy(xs.at[:, e, :, c[1]], xd.at[:, me, :, c[1]], 1, e, me, (e, j)))
        return out

    own_cols = (cols(j, 0, quarter), cols(far, 0, extra) if extra else None)

    def got_direct(i):
        out = [copy(xd.at[:, i, :, own_cols[0]], xd.at[:, i, :, own_cols[0]], 0, i, i, (i, j))]
        if extra:
            out.append(copy(xd.at[:, i, :, own_cols[1]], xd.at[:, i, :, own_cols[1]], 1, i, i, (i, j)))
        return out

    def sel_rows(a, e, src):
        return jnp.dot(sel[a, e], src[...], preferred_element_type=F32).astype(BF)

    def to_far(i):
        c = cols(j, extra, rest)
        return copy(xd.at[:, i, :, c], xd.at[:, i, :, c], 2, i, i, (me, far))

    def from_far(i):
        c = cols(far, extra, rest)
        return copy(xd.at[:, i, :, c], xd.at[:, i, :, c], 2, i, i, (me, far))

    def to_sib(i, mine):
        a, b = (j, far) if mine else (sib, farsib)
        c = cols(a, 0, quarter)
        out = [copy(xd.at[:, i, :, c], xd.at[:, i, :, c], 3, i, i, (me, sib))]
        if extra:
            c = cols(b, 0, extra)
            out.append(copy(xd.at[:, i, :, c], xd.at[:, i, :, c], 4, i, i, (me, sib)))
        return out

    def rest_sib(i, mine):
        c = cols(far if mine else farsib, extra, rest)
        return copy(xd.at[:, i, :, c], xd.at[:, i, :, c], 5, i, i, (me, sib))

    def step_a(i):
        return [copy(part.at[i, sib], ra.at[i, 0], 6, i, i, (me, sib)),
                copy(part.at[i, farsib], ra.at[i, 1], 7, i, i, (me, sib))]

    def step_b(i):
        return copy(sb.at[i], rb.at[i], 8, i, i, (me, far))

    def step_c(i):
        return copy(fb.at[i], ret.at[me], 9, i, me, (i, j))

    def got_c(i):
        return copy(fb.at[i], ret.at[i], 9, i, i, (i, j))

    def source(s):
        return lax.rem(me - s + n, n)

    def fill(s, carry):
        e = lax.rem(me + s, n)
        xs[0, e] = sel_rows(0, e, tok)
        xs[1, e] = sel_rows(1, e, cot)

        @pl.when(s == 1)
        def _():
            pl.semaphore_wait(barrier, n + 2)

        for c in direct(e, own_cols):
            c.start()
        return carry

    lax.fori_loop(1, n, fill, 0)
    xd[0, me] = sel_rows(0, me, tok)
    xd[1, me] = sel_rows(1, me, cot)
    for w in weights:
        w.wait()

    def f1(s):
        i = source(s)
        for c in got_direct(i):
            c.wait_recv()
        to_far(i).start()
        for c in to_sib(i, True):
            c.start()

    def f2(s):
        i = source(s)
        from_far(i).wait_recv()
        rest_sib(i, True).start()

    def f3(s):
        i = source(s)
        for c in to_sib(i, False):
            c.wait_recv()
        rest_sib(i, False).wait_recv()

    def expert(s):
        i = source(s)
        x = xd[0, i]
        a = jnp.dot(x, wg[...], preferred_element_type=F32)
        u = jnp.dot(x, wu[...], preferred_element_type=F32)
        q = lax.dot_general(xd[1, i], wd[...], INNER, preferred_element_type=F32)
        sig = jax.nn.sigmoid(a)
        act = a * sig
        h = (act * u).astype(BF)
        da = (q * u * sig * (1.0 + a * (1.0 - sig))).astype(BF)
        du = (q * act).astype(BF)
        hid[i] = h
        da_s[i] = da
        du_s[i] = du
        score = jnp.sum(h.astype(F32) * q, axis=1, keepdims=True)
        eye = (lax.broadcasted_iota(jnp.int32, (cap, 128), 0)
               == lax.broadcasted_iota(jnp.int32, (cap, 128), 1))
        row = jnp.sum(jnp.where(eye, score, 0.0), axis=0, keepdims=True)
        tile = jnp.broadcast_to(jnp.concatenate([row] * (quarter // 128), axis=1), (PAD, quarter)).astype(BF)
        for k in range(4):
            c = slice(k * quarter, (k + 1) * quarter)
            p = lax.dot_general(da, wg[c, :], INNER, preferred_element_type=F32)
            p = p + lax.dot_general(du, wu[c, :], INNER, preferred_element_type=F32)
            part[i, k, :cap, :] = p.astype(BF)
            part[i, k, cap:, :] = tile
        for c in step_a(i):
            c.start()

    def do_b(s):
        i = source(s)
        for c in step_a(i):
            c.wait_recv()
        sb[i] = (part[i, far].astype(F32) + ra[i, 1].astype(F32)).astype(BF)
        step_b(i).start()

    def do_c(s):
        i = source(s)
        step_b(i).wait_recv()
        total = (part[i, j].astype(F32) + ra[i, 0].astype(F32) + rb[i].astype(F32)).astype(BF)

        @pl.when(s == 0)
        def _():
            ret[me] = total

        @pl.when(s > 0)
        def _():
            fb[i] = total
            step_c(i).start()

    def main(t, carry):
        @pl.when(t > 0)
        def _():
            f3(t)

        expert(t)

        @pl.when(t == 0)
        def _():
            f1(1)

        @pl.when(t + 2 < n)
        def _():
            f1(t + 2)

        @pl.when(t + 1 < n)
        def _():
            f2(t + 1)

        @pl.when(t > 0)
        def _():
            do_b(t - 1)

        @pl.when(t > 1)
        def _():
            do_c(t - 2)

        return carry

    lax.fori_loop(0, n, main, 0)

    half = lax.broadcasted_iota(jnp.int32, (128, 128), 0) == lax.broadcasted_iota(jnp.int32, (128, 128), 1)

    def wgrad(c, carry):
        at = pl.ds(pl.multiple_of(c * chunk, chunk), chunk)
        rows = n * cap
        x = xd[0, :, :, at].reshape(rows, chunk)
        d = xd[1, :, :, at].reshape(rows, chunk)
        ff = hid.shape[2]
        g = lax.dot_general(x, da_s[...].reshape(rows, ff), OUTER, preferred_element_type=F32).astype(BF)
        gg[at, :] = g
        u = lax.dot_general(x, du_s[...].reshape(rows, ff), OUTER, preferred_element_type=F32).astype(BF)
        gu[at, :] = u
        gd[:, at] = lax.dot_general(hid[...].reshape(rows, ff), d, OUTER, preferred_element_type=F32).astype(BF)
        gw = g.astype(F32)
        uw = u.astype(F32)
        norm = jnp.sum(gw * gw + uw * uw, axis=1, keepdims=True)
        for k in range(chunk // 128):
            nrow[pl.ds(c * (chunk // 128) + k, 1), :] = jnp.sum(
                jnp.where(half, norm[k * 128:(k + 1) * 128], 0.0), axis=0, keepdims=True)

        @pl.when(c == 0)
        def _():
            do_b(n - 1)
            do_c(n - 2)

        @pl.when(c == 2)
        def _():
            do_c(n - 1)

        return carry

    lax.fori_loop(0, chunks, wgrad, 0)

    ntp[j] = nrow[...]

    def tp_copy(k, slot):
        return pltpu.make_async_remote_copy(
            src_ref=ntp.at[slot], dst_ref=ntp.at[slot], send_sem=ntps.at[k], recv_sem=ntpr.at[slot],
            device_id=(me, lax.rem(j + k, 4)), device_id_type=MESH)

    for k in range(1, 4):
        tp_copy(k, j).start()
    for k in range(1, 4):
        tp_copy(k, lax.rem(j + k, 4)).wait_recv()
    nep[me] = ntp[0] + ntp[1] + ntp[2] + ntp[3]

    def ep_copy(s, slot):
        return pltpu.make_async_remote_copy(
            src_ref=nep.at[slot], dst_ref=nep.at[slot], send_sem=neps.at[s], recv_sem=nepr.at[slot],
            device_id=(lax.rem(me + s, n), j), device_id_type=MESH)

    def ep_send(s, carry):
        ep_copy(s, me).start()
        return carry

    lax.fori_loop(1, n, ep_send, 0)

    def drain(s, carry):
        i = source(s)
        for c in direct(i, own_cols) + to_sib(i, True):
            c.wait_send()
        to_far(i).wait_send()
        rest_sib(i, True).wait_send()
        step_c(i).wait_send()
        got_c(i).wait_recv()
        return carry

    lax.fori_loop(1, n, drain, 0)

    def drain_tp(s, carry):
        i = source(s)
        for c in step_a(i):
            c.wait_send()
        step_b(i).wait_send()
        return carry

    lax.fori_loop(0, n, drain_tp, 0)

    def ep_wait(s, carry):
        ep_copy(s, lax.rem(me + s, n)).wait_recv()
        return carry

    lax.fori_loop(1, n, ep_wait, 0)
    nout[...] = lax.fori_loop(1, n, lambda i, acc: acc + nep[i], nep[0])

    def ep_drain(s, carry):
        ep_copy(s, me).wait_send()
        return carry

    lax.fori_loop(1, n, ep_drain, 0)
    for k in range(1, 4):
        tp_copy(k, j).wait_send()


def on_device(n, tokens, cotangent, routes, gate_weights, w_gate, w_up, w_down):
    tok_rows, width = tokens.shape
    top = routes.shape[1]
    ff = w_gate.shape[2]
    capacity = 2 * tok_rows * top // n
    cap = -(-capacity // 16) * 16
    quarter = width // 4
    rows = cap + PAD
    pairs = tok_rows * top

    flat = routes.reshape(-1)
    onehot = (flat[:, None] == jnp.arange(n, dtype=jnp.int32)[None, :]).astype(F32)
    ids = jnp.arange(pairs, dtype=jnp.int32)
    tri = (ids[None, :] < ids[:, None]).astype(BF)
    before = jnp.dot(tri, onehot.astype(BF), preferred_element_type=F32)
    position = jnp.sum(before * onehot, axis=1).astype(jnp.int32)
    slot = (flat * cap + position).reshape(tok_rows, top)
    gates = gate_weights.astype(BF)
    slots = jnp.arange(n * cap, dtype=jnp.int32)[:, None]
    hits = [slots == slot[:, k][None, :] for k in range(top)]
    pick = sum(h.astype(BF) for h in hits)
    pick_g = sum(jnp.where(h, gates[:, k][None, :], jnp.zeros((), BF)) for k, h in enumerate(hits))
    sel = jnp.stack([pick, pick_g]).reshape(2, n, cap, tok_rows)

    vmem = pl.BlockSpec(memory_space=pltpu.VMEM)
    anym = pl.BlockSpec(memory_space=pl.ANY)
    dma = pltpu.SemaphoreType.DMA
    ret, gg, gu, gd, norms = pl.pallas_call(
        functools.partial(kernel, n),
        out_shape=(
            jax.ShapeDtypeStruct((n, rows, quarter), BF),
            jax.ShapeDtypeStruct((width, ff), BF),
            jax.ShapeDtypeStruct((width, ff), BF),
            jax.ShapeDtypeStruct((ff, width), BF),
            jax.ShapeDtypeStruct((width // 128, 128), F32),
        ),
        in_specs=[vmem, vmem, vmem, anym, anym, anym],
        out_specs=(vmem, vmem, vmem, vmem, vmem),
        scratch_shapes=[
            pltpu.VMEM((width, ff), BF), pltpu.VMEM((width, ff), BF), pltpu.VMEM((ff, width), BF),
            pltpu.VMEM((2, n, cap, width), BF), pltpu.VMEM((2, n, cap, width), BF),
            pltpu.VMEM((n, cap, ff), BF), pltpu.VMEM((n, cap, ff), BF), pltpu.VMEM((n, cap, ff), BF),
            pltpu.VMEM((n, 4, rows, quarter), BF),
            pltpu.VMEM((n, 2, rows, quarter), BF),
            pltpu.VMEM((n, rows, quarter), BF), pltpu.VMEM((n, rows, quarter), BF),
            pltpu.VMEM((n, rows, quarter), BF),
            pltpu.VMEM((width // 128, 128), F32),
            pltpu.VMEM((4, width // 128, 128), F32), pltpu.VMEM((n, width // 128, 128), F32),
            dma((3,)), dma((10, n)), dma((10, n)), dma((4,)), dma((4,)), dma((n,)), dma((n,)),
        ],
        compiler_params=pltpu.CompilerParams(
            collective_id=0, has_side_effects=True, vmem_limit_bytes=62 * 1024 * 1024),
    )(sel, tokens, cotangent, w_gate[0], w_up[0], w_down[0])

    back = ret.reshape(n * rows, quarter)
    spot = flat * rows + position
    spots = jnp.arange(n * rows, dtype=jnp.int32)[None, :]
    spot2 = spot.reshape(tok_rows, top)
    comb = sum((spots == spot2[:, k][:, None]).astype(BF) for k in range(top))
    token_grad = jnp.dot(comb, back, preferred_element_type=F32).astype(BF)
    scores = ret[:, cap, :cap].reshape(1, n * cap).astype(F32)
    wanted = slot.reshape(pairs, 1) == jnp.arange(n * cap, dtype=jnp.int32)[None, :]
    score = jnp.sum(jnp.where(wanted, scores, 0.0), axis=1).reshape(tok_rows, top)
    score_grad = score / gates.astype(F32)
    return token_grad, score_grad, gg[None], gu[None], gd[None], norms.reshape(width)


def solution(mesh):
    return jax.shard_map(
        functools.partial(on_device, mesh.shape["ep"]),
        mesh=mesh,
        in_specs=(
            P("ep", None),
            P("ep", None),
            P("ep", None),
            P("ep", None),
            P("ep", None, "tp"),
            P("ep", None, "tp"),
            P("ep", "tp", None),
        ),
        out_specs=(
            P("ep", "tp"),
            P("ep", None),
            P("ep", None, "tp"),
            P("ep", None, "tp"),
            P("ep", "tp", None),
            P(),
        ),
        check_vma=False,
    )
```

```python
import functools

import jax
import jax.numpy as jnp
from jax import lax
from jax.experimental import pallas as pl
from jax.experimental.pallas import tpu as pltpu
from jax.sharding import PartitionSpec as P

MESH = pl.DeviceIdType.MESH
F32 = jnp.float32
BF = jnp.bfloat16
INNER = (((1,), (1,)), ((), ()))
OUTER = (((0,), (0,)), ((), ()))
PAD = 16
EXTRA = 2


def kernel(n, sel, tok, cot, wg_h, wu_h, wd_h, ret, gg, gu, gd, nout,
           wg, wu, wd, xs, xd, hid, da_s, du_s, part, ra, rb, sb, fb, nrow, ntp, nep,
           wsem, ssem, rsem, ntps, ntpr, neps, nepr):
    me = lax.axis_index("ep")
    j = lax.axis_index("tp")
    sib = j + 1 - 2 * lax.rem(j, 2)
    far = lax.rem(j + 2, 4)
    farsib = lax.rem(sib + 2, 4)
    cap = xd.shape[2]
    width = xd.shape[3]
    quarter = width // 4
    extra = EXTRA * 128
    rest = quarter - extra
    chunk = 256
    chunks = width // chunk

    weights = [pltpu.make_async_copy(src, dst, wsem.at[k])
               for k, (src, dst) in enumerate(((wg_h, wg), (wu_h, wu), (wd_h, wd)))]
    for w in weights:
        w.start()

    barrier = pltpu.get_barrier_semaphore()

    def greet(s, carry):
        pl.semaphore_signal(barrier, inc=1, device_id=(lax.rem(me + s, n), j), device_id_type=MESH)
        return carry

    lax.fori_loop(1, n, greet, 0)
    for k in range(1, 4):
        pl.semaphore_signal(barrier, inc=1, device_id=(me, lax.rem(j + k, 4)), device_id_type=MESH)

    def cols(q, start, size):
        return pl.ds(pl.multiple_of(q * quarter + start, 128), size)

    def copy(src, dst, kind, send_at, recv_at, dev):
        return pltpu.make_async_remote_copy(
            src_ref=src, dst_ref=dst, send_sem=ssem.at[kind, send_at],
            recv_sem=rsem.at[kind, recv_at], device_id=dev, device_id_type=MESH)

    def direct(e, c):
        out = [copy(xs.at[:, e, :, c[0]], xd.at[:, me, :, c[0]], 0, e, me, (e, j))]
        if extra:
            out.append(copy(xs.at[:, e, :, c[1]], xd.at[:, me, :, c[1]], 1, e, me, (e, j)))
        return out

    own_cols = (cols(j, 0, quarter), cols(far, 0, extra) if extra else None)

    def got_direct(i):
        out = [copy(xd.at[:, i, :, own_cols[0]], xd.at[:, i, :, own_cols[0]], 0, i, i, (i, j))]
        if extra:
            out.append(copy(xd.at[:, i, :, own_cols[1]], xd.at[:, i, :, own_cols[1]], 1, i, i, (i, j)))
        return out

    def sel_rows(a, e, src):
        return jnp.dot(sel[a, e], src[...], preferred_element_type=F32).astype(BF)

    def to_far(i):
        c = cols(j, extra, rest)
        return copy(xd.at[:, i, :, c], xd.at[:, i, :, c], 2, i, i, (me, far))

    def from_far(i):
        c = cols(far, extra, rest)
        return copy(xd.at[:, i, :, c], xd.at[:, i, :, c], 2, i, i, (me, far))

    def to_sib(i, mine):
        a, b = (j, far) if mine else (sib, farsib)
        c = cols(a, 0, quarter)
        out = [copy(xd.at[:, i, :, c], xd.at[:, i, :, c], 3, i, i, (me, sib))]
        if extra:
            c = cols(b, 0, extra)
            out.append(copy(xd.at[:, i, :, c], xd.at[:, i, :, c], 4, i, i, (me, sib)))
        return out

    def rest_sib(i, mine):
        c = cols(far if mine else farsib, extra, rest)
        return copy(xd.at[:, i, :, c], xd.at[:, i, :, c], 5, i, i, (me, sib))

    def step_a(i):
        return [copy(part.at[i, sib], ra.at[i, 0], 6, i, i, (me, sib)),
                copy(part.at[i, farsib], ra.at[i, 1], 7, i, i, (me, sib))]

    def step_b(i):
        return copy(sb.at[i], rb.at[i], 8, i, i, (me, far))

    def step_c(i):
        return copy(fb.at[i], ret.at[me], 9, i, me, (i, j))

    def got_c(i):
        return copy(fb.at[i], ret.at[i], 9, i, i, (i, j))

    def source(s):
        return lax.rem(me - s + n, n)

    def fill(s, carry):
        e = lax.rem(me + s, n)
        xs[0, e] = sel_rows(0, e, tok)
        xs[1, e] = sel_rows(1, e, cot)

        @pl.when(s == 1)
        def _():
            pl.semaphore_wait(barrier, n + 2)

        for c in direct(e, own_cols):
            c.start()
        return carry

    lax.fori_loop(1, n, fill, 0)
    xd[0, me] = sel_rows(0, me, tok)
    xd[1, me] = sel_rows(1, me, cot)
    for w in weights:
        w.wait()

    def f1(s):
        i = source(s)
        for c in got_direct(i):
            c.wait_recv()
        to_far(i).start()
        for c in to_sib(i, True):
            c.start()

    def f2(s):
        i = source(s)
        from_far(i).wait_recv()
        rest_sib(i, True).start()

    def f3(s):
        i = source(s)
        for c in to_sib(i, False):
            c.wait_recv()
        rest_sib(i, False).wait_recv()

    def expert(s):
        i = source(s)
        x = xd[0, i]
        a = lax.dot_general(x, wg[...], INNER, preferred_element_type=F32)
        u = lax.dot_general(x, wu[...], INNER, preferred_element_type=F32)
        q = lax.dot_general(xd[1, i], wd[...], INNER, preferred_element_type=F32)
        sig = jax.nn.sigmoid(a)
        act = a * sig
        h = (act * u).astype(BF)
        da = (q * u * sig * (1.0 + a * (1.0 - sig))).astype(BF)
        du = (q * act).astype(BF)
        hid[i] = h
        da_s[i] = da
        du_s[i] = du
        score = jnp.sum(h.astype(F32) * q, axis=1, keepdims=True)
        eye = (lax.broadcasted_iota(jnp.int32, (cap, 128), 0)
               == lax.broadcasted_iota(jnp.int32, (cap, 128), 1))
        row = jnp.sum(jnp.where(eye, score, 0.0), axis=0, keepdims=True)
        tile = jnp.broadcast_to(jnp.concatenate([row] * (quarter // 128), axis=1), (PAD, quarter)).astype(BF)
        for k in range(4):
            c = slice(k * quarter, (k + 1) * quarter)
            p = jnp.dot(da, wg[:, c], preferred_element_type=F32)
            p = p + jnp.dot(du, wu[:, c], preferred_element_type=F32)
            part[i, k, :cap, :] = p.astype(BF)
            part[i, k, cap:, :] = tile
        for c in step_a(i):
            c.start()

    def do_b(s):
        i = source(s)
        for c in step_a(i):
            c.wait_recv()
        sb[i] = (part[i, far].astype(F32) + ra[i, 1].astype(F32)).astype(BF)
        step_b(i).start()

    def do_c(s):
        i = source(s)
        step_b(i).wait_recv()
        total = (part[i, j].astype(F32) + ra[i, 0].astype(F32) + rb[i].astype(F32)).astype(BF)

        @pl.when(s == 0)
        def _():
            ret[me] = total

        @pl.when(s > 0)
        def _():
            fb[i] = total
            step_c(i).start()

    def main(t, carry):
        @pl.when(t > 0)
        def _():
            f3(t)

        expert(t)

        @pl.when(t == 0)
        def _():
            f1(1)

        @pl.when(t + 2 < n)
        def _():
            f1(t + 2)

        @pl.when(t + 1 < n)
        def _():
            f2(t + 1)

        @pl.when(t > 0)
        def _():
            do_b(t - 1)

        @pl.when(t > 1)
        def _():
            do_c(t - 2)

        return carry

    lax.fori_loop(0, n, main, 0)

    def wgrad(c, carry):
        at = pl.ds(pl.multiple_of(c * chunk, chunk), chunk)
        rows = n * cap
        x = xd[0, :, :, at].reshape(rows, chunk)
        d = xd[1, :, :, at].reshape(rows, chunk)
        ff = hid.shape[2]
        g = lax.dot_general(da_s[...].reshape(rows, ff), x, OUTER, preferred_element_type=F32).astype(BF)
        gg[:, at] = g
        u = lax.dot_general(du_s[...].reshape(rows, ff), x, OUTER, preferred_element_type=F32).astype(BF)
        gu[:, at] = u
        gd[:, at] = lax.dot_general(hid[...].reshape(rows, ff), d, OUTER, preferred_element_type=F32).astype(BF)
        gw = g.astype(F32)
        uw = u.astype(F32)
        norm = jnp.sum(gw * gw + uw * uw, axis=0, keepdims=True)
        for k in range(chunk // 128):
            nrow[pl.ds(c * (chunk // 128) + k, 1), :] = norm[:, k * 128:(k + 1) * 128]

        @pl.when(c == 0)
        def _():
            do_b(n - 1)
            do_c(n - 2)

        @pl.when(c == 2)
        def _():
            do_c(n - 1)

        return carry

    lax.fori_loop(0, chunks, wgrad, 0)

    ntp[j] = nrow[...]

    def tp_copy(k, slot):
        return pltpu.make_async_remote_copy(
            src_ref=ntp.at[slot], dst_ref=ntp.at[slot], send_sem=ntps.at[k], recv_sem=ntpr.at[slot],
            device_id=(me, lax.rem(j + k, 4)), device_id_type=MESH)

    for k in range(1, 4):
        tp_copy(k, j).start()
    for k in range(1, 4):
        tp_copy(k, lax.rem(j + k, 4)).wait_recv()
    nep[me] = ntp[0] + ntp[1] + ntp[2] + ntp[3]

    def ep_copy(s, slot):
        return pltpu.make_async_remote_copy(
            src_ref=nep.at[slot], dst_ref=nep.at[slot], send_sem=neps.at[s], recv_sem=nepr.at[slot],
            device_id=(lax.rem(me + s, n), j), device_id_type=MESH)

    def ep_send(s, carry):
        ep_copy(s, me).start()
        return carry

    lax.fori_loop(1, n, ep_send, 0)

    def drain(s, carry):
        i = source(s)
        for c in direct(i, own_cols) + to_sib(i, True):
            c.wait_send()
        to_far(i).wait_send()
        rest_sib(i, True).wait_send()
        step_c(i).wait_send()
        got_c(i).wait_recv()
        return carry

    lax.fori_loop(1, n, drain, 0)

    def drain_tp(s, carry):
        i = source(s)
        for c in step_a(i):
            c.wait_send()
        step_b(i).wait_send()
        return carry

    lax.fori_loop(0, n, drain_tp, 0)

    def ep_wait(s, carry):
        ep_copy(s, lax.rem(me + s, n)).wait_recv()
        return carry

    lax.fori_loop(1, n, ep_wait, 0)
    nout[...] = lax.fori_loop(1, n, lambda i, acc: acc + nep[i], nep[0])

    def ep_drain(s, carry):
        ep_copy(s, me).wait_send()
        return carry

    lax.fori_loop(1, n, ep_drain, 0)
    for k in range(1, 4):
        tp_copy(k, j).wait_send()


def on_device(n, tokens, cotangent, routes, gate_weights, w_gate, w_up, w_down):
    tok_rows, width = tokens.shape
    top = routes.shape[1]
    ff = w_gate.shape[2]
    capacity = 2 * tok_rows * top // n
    cap = -(-capacity // 16) * 16
    quarter = width // 4
    rows = cap + PAD
    pairs = tok_rows * top

    flat = routes.reshape(-1)
    onehot = (flat[:, None] == jnp.arange(n, dtype=jnp.int32)[None, :]).astype(F32)
    ids = jnp.arange(pairs, dtype=jnp.int32)
    tri = (ids[None, :] < ids[:, None]).astype(BF)
    before = jnp.dot(tri, onehot.astype(BF), preferred_element_type=F32)
    position = jnp.sum(before * onehot, axis=1).astype(jnp.int32)
    slot = (flat * cap + position).reshape(tok_rows, top)
    gates = gate_weights.astype(BF)
    slots = jnp.arange(n * cap, dtype=jnp.int32)[:, None]
    hits = [slots == slot[:, k][None, :] for k in range(top)]
    pick = sum(h.astype(BF) for h in hits)
    pick_g = sum(jnp.where(h, gates[:, k][None, :], jnp.zeros((), BF)) for k, h in enumerate(hits))
    sel = jnp.stack([pick, pick_g]).reshape(2, n, cap, tok_rows)

    vmem = pl.BlockSpec(memory_space=pltpu.VMEM)
    anym = pl.BlockSpec(memory_space=pl.ANY)
    dma = pltpu.SemaphoreType.DMA
    ret, gg, gu, gd, norms = pl.pallas_call(
        functools.partial(kernel, n),
        out_shape=(
            jax.ShapeDtypeStruct((n, rows, quarter), BF),
            jax.ShapeDtypeStruct((ff, width), BF),
            jax.ShapeDtypeStruct((ff, width), BF),
            jax.ShapeDtypeStruct((ff, width), BF),
            jax.ShapeDtypeStruct((width // 128, 128), F32),
        ),
        in_specs=[vmem, vmem, vmem, anym, anym, anym],
        out_specs=(vmem, vmem, vmem, vmem, vmem),
        scratch_shapes=[
            pltpu.VMEM((ff, width), BF), pltpu.VMEM((ff, width), BF), pltpu.VMEM((ff, width), BF),
            pltpu.VMEM((2, n, cap, width), BF), pltpu.VMEM((2, n, cap, width), BF),
            pltpu.VMEM((n, cap, ff), BF), pltpu.VMEM((n, cap, ff), BF), pltpu.VMEM((n, cap, ff), BF),
            pltpu.VMEM((n, 4, rows, quarter), BF),
            pltpu.VMEM((n, 2, rows, quarter), BF),
            pltpu.VMEM((n, rows, quarter), BF), pltpu.VMEM((n, rows, quarter), BF),
            pltpu.VMEM((n, rows, quarter), BF),
            pltpu.VMEM((width // 128, 128), F32),
            pltpu.VMEM((4, width // 128, 128), F32), pltpu.VMEM((n, width // 128, 128), F32),
            dma((3,)), dma((10, n)), dma((10, n)), dma((4,)), dma((4,)), dma((n,)), dma((n,)),
        ],
        compiler_params=pltpu.CompilerParams(
            collective_id=0, has_side_effects=True, vmem_limit_bytes=62 * 1024 * 1024),
    )(sel, tokens, cotangent, w_gate[0].T, w_up[0].T, w_down[0])

    back = ret.reshape(n * rows, quarter)
    spot = flat * rows + position
    spots = jnp.arange(n * rows, dtype=jnp.int32)[None, :]
    spot2 = spot.reshape(tok_rows, top)
    comb = sum((spots == spot2[:, k][:, None]).astype(BF) for k in range(top))
    token_grad = jnp.dot(comb, back, preferred_element_type=F32).astype(BF)
    scores = ret[:, cap, :cap].reshape(1, n * cap).astype(F32)
    wanted = slot.reshape(pairs, 1) == jnp.arange(n * cap, dtype=jnp.int32)[None, :]
    score = jnp.sum(jnp.where(wanted, scores, 0.0), axis=1).reshape(tok_rows, top)
    score_grad = score / gates.astype(F32)
    return token_grad, score_grad, gg.T[None], gu.T[None], gd[None], norms.reshape(width)


def solution(mesh):
    return jax.shard_map(
        functools.partial(on_device, mesh.shape["ep"]),
        mesh=mesh,
        in_specs=(
            P("ep", None),
            P("ep", None),
            P("ep", None),
            P("ep", None),
            P("ep", None, "tp"),
            P("ep", None, "tp"),
            P("ep", "tp", None),
        ),
        out_specs=(
            P("ep", "tp"),
            P("ep", None),
            P("ep", None, "tp"),
            P("ep", None, "tp"),
            P("ep", "tp", None),
            P(),
        ),
        check_vma=False,
    )
```
